32 devices in a mesh: grp: 2 (over y), sp: 4 (over z), tp: 4 (over x, core).
Axes of the slice: x: 2, y: 2, z: 4, core: 2. Of those that a mesh axis runs over, the one named last changes fastest.
Arguments:
- residual: bfloat16 [2048, 2048], P(('grp', 'sp', 'tp')), parts along dimension 0, may hold values from -6 to 6
- queries_wide: bfloat16 [2048, 1024], P(('grp', 'sp'), 'tp'), parts along dimension 0, may hold values from -6 to 6
- keys_wide: bfloat16 [2048, 512], P(('grp', 'sp'), 'tp'), parts along dimension 0, may hold values from -6 to 6
- values_wide: bfloat16 [2048, 512], P(('grp', 'sp'), 'tp'), parts along dimension 0, may hold values from -6 to 6
- queries_narrow: bfloat16 [2048, 512], P(('grp', 'sp'), 'tp'), parts along dimension 0, may hold values from -6 to 6
- keys_narrow: bfloat16 [2048, 256], P(('grp', 'sp'), 'tp'), parts along dimension 0, may hold values from -6 to 6
- values_narrow: bfloat16 [2048, 256], P(('grp', 'sp'), 'tp'), parts along dimension 0, may hold values from -6 to 6
- query_gain_wide: float32 [128], replicated, may hold values from 1 to 6
- key_gain_wide: float32 [128], replicated, may hold values from 1 to 6
- query_gain_narrow: float32 [64], replicated, may hold values from 1 to 6
- key_gain_narrow: float32 [64], replicated, may hold values from 1 to 6
- output_wide: bfloat16 [1024, 2048], P('tp'), may hold values from -0.3125 to 0.3125
- output_narrow: bfloat16 [512, 2048], P('tp'), may hold values from -0.3125 to 0.3125
- norm_gain: float32 [2048], replicated, may hold values from 0.1 to 1.9
- gate_weight: bfloat16 [4, 2048, 3584], P('sp', None, 'tp'), may hold values from -0.125 to 0.125
- up_weight: bfloat16 [4, 2048, 3584], P('sp', None, 'tp'), may hold values from -0.125 to 0.125
- down_weight: bfloat16 [4, 3584, 2048], P('sp', 'tp'), may hold values from -0.09375 to 0.09375
- route_ids: int32 [2048, 2], P(('grp', 'sp', 'tp')), parts along dimension 0, may hold values from 0 to 3, all different within a row; in each aligned block of 64 rows (0 to 63, 64 to 127, ...) at most 64 rows name the same one
- route_weights: float32 [2048, 2], P(('grp', 'sp', 'tp')), parts along dimension 0, may hold values from 0.1 to 0.9
Outputs:
- result: bfloat16 [2048, 2048], P(('grp', 'sp', 'tp')), parts along dimension 0
The draws below stay inside these ranges and needn't reach their ends.
There are 2 independent parts, one for each index of `grp`. The reference program is written for one: setup_inputs(seed, part) draws one part's arguments, and reference() takes and returns one part's arrays. A program takes and returns all parts, laid end to end along the dimension named above; an argument that names none is the same for every part. Nothing has to cross between parts.
Inputs may be any that keep to these rules, and one draw needn't show every extreme that they name: `route_ids`: in each aligned block of 64 rows (the rows of one device) no expert is named by more than 64 rows, a bound that some block reaches; a row names 2 different experts.
All inputs are finite; a program needn't handle non-finite values.
Results may differ from the reference program's by a relative error of at most 0.013.
The reference program's roundings to bfloat16 on the way count: a program that leaves them out, or rounds other values in their place, can miss the bound.
Values may be sent and summed in bfloat16 or wider, within the bound.
A program may use at most 128 MiB of HBM per device.

```python
import math
import jax
import jax.numpy as jnp
import numpy as np
from jax import lax

D = 2048
HW = 8
KW = 4
DW = 128
HN = 8
KN = 4
DN = 64
FF = 3584
TOPK = 2
GRID = 64
TOKENS = 1024
ROWS = 64
EXPERTS = 4
CAP = 64
N_SP = 4
N_TP = 4


def draw_field(key, tag, head_count, head_width):
    noise_key = jax.random.fold_in(key, tag)
    field = jax.random.normal(noise_key, (TOKENS, head_count, head_width), jnp.float32)
    field = jnp.clip(field, -6.0, 6.0)
    return field.reshape(TOKENS, head_count * head_width).astype(jnp.bfloat16)


def draw_gain(key, tag, head_width):
    base_key = jax.random.fold_in(key, tag)
    return jax.random.uniform(base_key, (head_width,), jnp.float32, 1.0, 2.2)


def draw_queries_wide(key, part):
    return draw_field(key, 101, HW, DW)


def draw_keys_wide(key, part):
    return draw_field(key, 102, KW, DW)


def draw_queries_narrow(key, part):
    return draw_field(key, 103, HN, DN)


def draw_keys_narrow(key, part):
    return draw_field(key, 104, KN, DN)


def draw_query_gain_wide(key, part):
    return draw_gain(key, 201, DW)


def draw_key_gain_wide(key, part):
    return draw_gain(key, 202, DW)


def draw_query_gain_narrow(key, part):
    return draw_gain(key, 203, DN)


def draw_key_gain_narrow(key, part):
    return draw_gain(key, 204, DN)


def block_scale(key, dims, split, smallest, largest):
    gain = 1.0
    for dim, shards_of in split:
        heights = jax.random.uniform(jax.random.fold_in(jax.random.fold_in(key, 6), dim), (shards_of,), jnp.float32, smallest / len(split), largest / len(split))
        gain = gain * jnp.repeat(jnp.exp(heights), dims[dim] // shards_of).reshape((-1,) + (1,) * (len(dims) - 1 - dim))
    return gain


def shared_out(stream_key, own, number, rows, count, top, limit, skew):
    sequence = jax.random.permutation(stream_key, count)
    packed, usual = shares(count, rows * top, limit, skew, True), shares(count, rows * top, limit, skew, False)
    places = jnp.arange(count)

    def named(sizes, rotation):
        used = int((sizes > 0).sum())
        fixed = max(1, used // 4)
        moved = fixed + (places - fixed + rotation * (used - fixed)) % max(1, count - fixed)
        return jnp.zeros((count,), jnp.int32).at[sequence[jnp.where(places < fixed, places, moved)]].set(jnp.asarray(sizes, jnp.int32))

    sizes = jnp.where(number % 4 == 0, named(packed, number // 4), named(usual, number - number // 4 - 1))
    mixed = jax.random.permutation(jax.random.fold_in(own, 3), count)
    source_of, receiver = mixed[0:count // 2 * 2:2], mixed[1:count // 2 * 2:2]
    margin = jnp.minimum(sizes[source_of] - 1, limit - sizes[receiver]) // 2
    margin = jnp.where((source_of == sequence[0]) | (receiver == sequence[0]) | (sizes[receiver] == 0), 0, jnp.maximum(margin, 0))
    moved = jax.random.randint(jax.random.fold_in(own, 4), (count // 2,), 0, 1 << 20) % (margin + 1)
    sizes = sizes.at[source_of].add(-moved).at[receiver].add(moved)
    items = jnp.searchsorted(jnp.cumsum(sizes), jnp.arange(rows * top), side="right").astype(jnp.int32)
    grid = items.reshape(top, rows).T
    grid = grid[jax.random.permutation(jax.random.fold_in(own, 1), rows)]
    rotation = jax.random.randint(jax.random.fold_in(own, 2), (rows, 1), 0, top)
    return jnp.take_along_axis(grid, (jnp.arange(top)[None, :] + rotation) % top, axis=1)


def shares(amount, total, bound, slope, full):
    portions = [(1 << 20) // math.isqrt(grade ** slope) + 1 for grade in range(1, amount + 1)]
    largest = bound if full else min(bound, max(-(-total // amount), total * portions[0] // sum(portions)))
    least = 1 if total - largest >= amount - 1 else 0
    counts, spare = [largest] + [least] * (amount - 1), total - largest - least * (amount - 1)
    while spare > 0:
        candidates = [i for i in range(1, amount) if counts[i] < largest] or [i for i in range(1, amount) if counts[i] < bound]
        mass, left = sum([portions[i] for i in candidates]), spare
        for i in candidates:
            more = min(bound - counts[i], max(1, left * portions[i] // mass), spare)
            counts[i] = counts[i] + more
            spare = spare - more
    return np.array(counts)


def noise(rng, shape, width, reach, split=(), kind=jnp.bfloat16):
    level = block_scale(rng, shape, split, -0.22, 0.18) if split else 1.0
    result = jax.random.normal(rng, shape, jnp.float32) * width * level
    return jnp.minimum(jnp.maximum(result, -reach), reach).astype(kind)


def setup_inputs(seed: int = 0, part: int = 0) -> dict:
    splits = jax.random.split(jax.random.key(seed), 20)
    part_splits = jax.random.split(jax.random.fold_in(splits[19], part), 20)
    residual = noise(part_splits[0], (TOKENS, D), 1.0, 6.0, ((0, 16),))
    queries_wide = draw_queries_wide(jax.random.fold_in(jax.random.fold_in(splits[19], part), 71), part)
    keys_wide = draw_keys_wide(jax.random.fold_in(jax.random.fold_in(splits[19], part), 71), part)
    values_wide = noise(part_splits[3], (TOKENS, KW * DW), 1.0, 6.0, ((0, 4), (1, 4)))
    queries_narrow = draw_queries_narrow(jax.random.fold_in(jax.random.fold_in(splits[19], part), 71), part)
    keys_narrow = draw_keys_narrow(jax.random.fold_in(jax.random.fold_in(splits[19], part), 71), part)
    values_narrow = noise(part_splits[6], (TOKENS, KN * DN), 1.0, 6.0, ((0, 4), (1, 4)))
    query_gain_wide = draw_query_gain_wide(jax.random.fold_in(splits[19], 71), part)
    key_gain_wide = draw_key_gain_wide(jax.random.fold_in(splits[19], 71), part)
    query_gain_narrow = draw_query_gain_narrow(jax.random.fold_in(splits[19], 71), part)
    key_gain_narrow = draw_key_gain_narrow(jax.random.fold_in(splits[19], 71), part)
    output_wide = noise(splits[11], (HW * DW, D), ((HW * DW + HN * DN) // 4) ** -0.5, 0.3125, ((0, 4),))
    output_narrow = noise(splits[12], (HN * DN, D), ((HW * DW + HN * DN) // 4) ** -0.5, 0.3125, ((0, 4),))
    norm_gain = jnp.clip(1.0 + 0.18 * jax.random.normal(splits[13], (D,), jnp.float32), 0.1, 1.9)
    gate_weight = noise(splits[14], (EXPERTS, D, FF), D ** -0.5, 0.125, ((0, 4), (2, 4)))
    up_weight = noise(splits[15], (EXPERTS, D, FF), D ** -0.5, 0.125, ((0, 4), (2, 4)))
    down_weight = noise(splits[16], (EXPERTS, FF, D), FF ** -0.5, 0.09375, ((0, 4), (1, 4)))
    route_ids_keys = jax.random.split(jax.random.fold_in(part_splits[17], 1), TOKENS // ROWS)
    route_ids_turns = jax.random.permutation(jax.random.fold_in(part_splits[17], 3), TOKENS // ROWS)
    route_ids = jax.vmap(lambda own, number: shared_out(jax.random.fold_in(part_splits[17], 2), own, number, ROWS, EXPERTS, TOPK, CAP, 2))(route_ids_keys, route_ids_turns).reshape((TOKENS, TOPK))
    route_weights = jnp.clip(0.1 + 0.79999997 * jax.random.uniform(part_splits[18], (TOKENS, TOPK), jnp.float32) ** block_scale(part_splits[18], (TOKENS, TOPK), ((0, 16),), -0.2, 0.2), 0.1, 0.9)
    return {"residual": residual, "queries_wide": queries_wide, "keys_wide": keys_wide, "values_wide": values_wide, "queries_narrow": queries_narrow, "keys_narrow": keys_narrow, "values_narrow": values_narrow, "query_gain_wide": query_gain_wide, "key_gain_wide": key_gain_wide, "query_gain_narrow": query_gain_narrow, "key_gain_narrow": key_gain_narrow, "output_wide": output_wide, "output_narrow": output_narrow, "norm_gain": norm_gain, "gate_weight": gate_weight, "up_weight": up_weight, "down_weight": down_weight, "route_ids": route_ids, "route_weights": route_weights}


THETA = 10000.0
EPS = 1e-06

def rotary_tables(places, head_width):
    quarter = head_width // 4
    inv_freq = THETA ** (-jnp.arange(quarter, dtype=jnp.float32) / quarter)
    grid_rows = (places // GRID).astype(jnp.float32)
    grid_cols = (places % GRID).astype(jnp.float32)
    row_angle = grid_rows[:, None] * inv_freq[None, :]
    col_angle = grid_cols[:, None] * inv_freq[None, :]
    angles = jnp.concatenate([row_angle, row_angle, col_angle, col_angle], axis=-1)
    return (jnp.cos(angles), jnp.sin(angles))

def head_norm_rotate(values, gain_vec, cos_table, sin_table):
    as_float = values.astype(jnp.float32)
    scaled = as_float * lax.rsqrt(lax.optimization_barrier(jnp.mean(as_float * as_float, axis=-1, keepdims=True)) + EPS)
    scaled = scaled * gain_vec.astype(jnp.float32)
    full_shape = scaled.shape
    quarter = full_shape[-1] // 4
    halves = scaled.reshape(full_shape[:-1] + (2, 2, quarter))
    turned = jnp.stack([-halves[..., 1, :], halves[..., 0, :]], axis=-2).reshape(full_shape)
    return (scaled * cos_table[:, None, :] + turned * sin_table[:, None, :]).astype(jnp.bfloat16)

def rounded(values):
    return lax.optimization_barrier(values.astype(jnp.bfloat16)).astype(jnp.float32)

def attend(queries, keys, values, key_heads):
    token_count = queries.shape[0]
    head_width = queries.shape[2]
    group_size = queries.shape[1] // key_heads
    block_len = math.gcd(token_count, 512)
    grouped = queries.reshape(token_count // block_len, block_len, key_heads, group_size, head_width)
    keys_float = keys.reshape(token_count, key_heads, head_width).astype(jnp.float32)
    values_float = values.reshape(token_count, key_heads, head_width).astype(jnp.float32)
    score_scale = head_width ** (-0.5)

    def one_block(query_block):
        scores = jnp.einsum('qhgd,khd->hgqk', query_block.astype(jnp.float32), keys_float) * score_scale
        row_max = lax.optimization_barrier(jnp.max(scores, axis=-1, keepdims=True))
        weights = jnp.exp(scores - row_max)
        weight_sum = lax.optimization_barrier(jnp.sum(weights, axis=-1))
        mixed_values = jnp.einsum('hgqk,khd->qhgd', rounded(weights), values_float)
        return (mixed_values / jnp.transpose(weight_sum, (2, 0, 1))[..., None]).astype(jnp.bfloat16)
    heads_out = lax.map(one_block, grouped)
    return heads_out.reshape(token_count, key_heads * group_size * head_width)

def reference(residual, queries_wide, keys_wide, values_wide, queries_narrow, keys_narrow, values_narrow, query_gain_wide, key_gain_wide, query_gain_narrow, key_gain_narrow, output_wide, output_narrow, norm_gain, gate_weight, up_weight, down_weight, route_ids, route_weights):
    places = jnp.arange(TOKENS, dtype=jnp.int32)
    cos_wide, sin_wide = rotary_tables(places, DW)
    cos_narrow, sin_narrow = rotary_tables(places, DN)
    q_wide = head_norm_rotate(queries_wide.reshape(TOKENS, HW, DW), query_gain_wide, cos_wide, sin_wide)
    k_wide = head_norm_rotate(keys_wide.reshape(TOKENS, KW, DW), key_gain_wide, cos_wide, sin_wide)
    q_narrow = head_norm_rotate(queries_narrow.reshape(TOKENS, HN, DN), query_gain_narrow, cos_narrow, sin_narrow)
    k_narrow = head_norm_rotate(keys_narrow.reshape(TOKENS, KN, DN), key_gain_narrow, cos_narrow, sin_narrow)
    heads_wide = attend(q_wide, k_wide, values_wide, KW)
    heads_narrow = attend(q_narrow, k_narrow, values_narrow, KN)
    wide_cols = HW * DW // N_TP
    narrow_cols = HN * DN // N_TP
    summed = jnp.zeros((TOKENS, D), jnp.float32)
    for shard_index in range(N_TP):
        wide_lo = shard_index * wide_cols
        narrow_lo = shard_index * narrow_cols
        shard_term = jnp.dot(heads_wide[:, wide_lo:wide_lo + wide_cols], output_wide[wide_lo:wide_lo + wide_cols], preferred_element_type=jnp.float32)
        shard_term = shard_term + jnp.dot(heads_narrow[:, narrow_lo:narrow_lo + narrow_cols], output_narrow[narrow_lo:narrow_lo + narrow_cols], preferred_element_type=jnp.float32)
        summed = summed + rounded(shard_term)
    state_float = rounded(residual.astype(jnp.float32) + summed)
    normed = (state_float * lax.rsqrt(lax.optimization_barrier(jnp.mean(state_float * state_float, axis=-1, keepdims=True)) + EPS) * norm_gain.astype(jnp.float32)).astype(jnp.bfloat16)
    flat_ids = route_ids.reshape(-1)
    flat_weights = route_weights.reshape(-1)
    room = N_SP * N_TP * CAP
    shard_cols = FF // N_TP

    def expert_step(carried, expert):
        gate_one, up_one, down_one, number = expert
        ordering = jnp.argsort((flat_ids != number).astype(jnp.int32), stable=True)[:room].astype(jnp.int32)
        live_slot = flat_ids[ordering] == number
        owner_row = ordering // TOPK
        picked = normed[owner_row]
        gate_act = jnp.dot(picked, gate_one, preferred_element_type=jnp.float32)
        up_act = jnp.dot(picked, up_one, preferred_element_type=jnp.float32)
        hidden = (jax.nn.silu(gate_act) * up_act).astype(jnp.bfloat16)
        summed_out = jnp.zeros((room, D), jnp.float32)
        for shard_index in range(N_TP):
            low = shard_index * shard_cols
            partial_value = jnp.dot(hidden[:, low:low + shard_cols], down_one[low:low + shard_cols], preferred_element_type=jnp.float32)
            summed_out = summed_out + rounded(partial_value)
        expert_out = rounded(summed_out)
        weight = jnp.where(live_slot, flat_weights[ordering], 0.0)
        return (carried.at[owner_row].add(weight[:, None] * expert_out), None)
    mixture, _ = lax.scan(expert_step, jnp.zeros((TOKENS, D), jnp.float32), (gate_weight, up_weight, down_weight, jnp.arange(EXPERTS, dtype=jnp.int32)))
    return (state_float + mixture).astype(jnp.bfloat16)
```

```python
import functools

import jax
import jax.numpy as jnp
import numpy as np
from jax import lax
from jax.experimental import pallas as pl
from jax.experimental.pallas import tpu as pltpu
from jax.sharding import PartitionSpec as P

GRID = 64


THETA = 10000.0
EPS = 1e-06
NEG_BIG = -1e30


def rotary_tables(places, head_width):
    quarter = head_width // 4
    inv_freq = THETA ** (-jnp.arange(quarter, dtype=jnp.float32) / quarter)
    grid_rows = (places // GRID).astype(jnp.float32)
    grid_cols = (places % GRID).astype(jnp.float32)
    row_angle = grid_rows[:, None] * inv_freq[None, :]
    col_angle = grid_cols[:, None] * inv_freq[None, :]
    angles = jnp.concatenate([row_angle, row_angle, col_angle, col_angle], axis=-1)
    return (jnp.cos(angles), jnp.sin(angles))


def head_norm_rotate(values, gain_vec, cos_table, sin_table):
    as_float = values.astype(jnp.float32)
    scaled = as_float * lax.rsqrt(jnp.mean(as_float * as_float, axis=-1, keepdims=True) + EPS)
    scaled = scaled * gain_vec
    full_shape = scaled.shape
    quarter = full_shape[-1] // 4
    halves = scaled.reshape(full_shape[:-1] + (2, 2, quarter))
    turned = jnp.stack([-halves[..., 1, :], halves[..., 0, :]], axis=-2).reshape(full_shape)
    return (scaled * cos_table[:, None, :] + turned * sin_table[:, None, :]).astype(jnp.bfloat16)


def fresh_state(queries):
    key_heads, group_size, tok_count = (queries.shape[1], queries.shape[2], queries.shape[0])
    return (
        jnp.full((key_heads, group_size, tok_count), NEG_BIG, jnp.float32),
        jnp.zeros((key_heads, group_size, tok_count), jnp.float32),
        jnp.zeros(queries.shape, jnp.float32),
    )


def key_sweep(carried, queries, keys, values):
    key_count = keys.shape[0]
    key_heads = queries.shape[1]
    head_width = queries.shape[3]
    block_len = 2048 if key_count % 2048 == 0 else key_count
    key_blocks = keys.reshape(key_count // block_len, block_len, key_heads, head_width)
    value_blocks = values.reshape(key_count // block_len, block_len, key_heads, head_width)
    score_scale = head_width ** (-0.5)

    def step(carried_state, blocks_in):
        key_block, value_block = blocks_in
        running_max, weight_sum, weighted = carried_state
        scores = (
            jnp.einsum("qhgd,khd->hgqk", queries, key_block, preferred_element_type=jnp.float32)
            * score_scale
        )
        new_max = jnp.maximum(running_max, jnp.max(scores, axis=-1))
        weights = jnp.exp(scores - new_max[..., None])
        rescale = jnp.exp(running_max - new_max)
        weight_sum = weight_sum * rescale + jnp.sum(weights, axis=-1)
        mixed_values = jnp.einsum(
            "hgqk,khd->qhgd",
            weights.astype(jnp.bfloat16),
            value_block,
            preferred_element_type=jnp.float32,
        )
        weighted = weighted * jnp.transpose(rescale, (2, 0, 1))[..., None] + mixed_values
        return ((new_max, weight_sum, weighted), None)

    carried, _ = lax.scan(step, carried, (key_blocks, value_blocks))
    return carried


def finish_heads(carried):
    weighted = carried[2]
    outcome = weighted / jnp.transpose(carried[1], (2, 0, 1))[..., None]
    return outcome.astype(jnp.bfloat16).reshape(weighted.shape[0], -1)


def slot_tables(chosen, slot_count, expert_count):
    row_count = chosen.shape[0]
    pick_count = chosen.shape[1]
    flat_pick = chosen.reshape(row_count * pick_count)
    hit_marks = (flat_pick[:, None] == jnp.arange(expert_count, dtype=jnp.int32)[None, :]).astype(
        jnp.int32
    )
    before = jnp.cumsum(hit_marks, axis=0) - hit_marks
    slot_place = jnp.sum(before * hit_marks, axis=1)
    target = flat_pick * slot_count + slot_place
    slot_table = target[:, None] == jnp.arange(expert_count * slot_count, dtype=jnp.int32)[None, :]
    return slot_table.astype(jnp.bfloat16).reshape(row_count, pick_count, expert_count * slot_count)


def plain_body(
    residual,
    queries_wide,
    keys_wide,
    values_wide,
    queries_narrow,
    keys_narrow,
    values_narrow,
    query_gain_wide,
    key_gain_wide,
    query_gain_narrow,
    key_gain_narrow,
    output_wide,
    output_narrow,
    norm_gain,
    gate_weight,
    up_weight,
    down_weight,
    route_ids,
    route_weights,
):
    tok_count = queries_wide.shape[0]
    places = lax.axis_index("sp") * tok_count + jnp.arange(tok_count, dtype=jnp.int32)
    wide_width = query_gain_wide.shape[0]
    narrow_width = query_gain_narrow.shape[0]
    cos_wide, sin_wide = rotary_tables(places, wide_width)
    cos_narrow, sin_narrow = rotary_tables(places, narrow_width)
    wide_keyheads = keys_wide.shape[1] // wide_width
    narrow_keyheads = keys_narrow.shape[1] // narrow_width
    q_wide = head_norm_rotate(
        queries_wide.reshape(tok_count, -1, wide_width), query_gain_wide, cos_wide, sin_wide
    )
    q_wide = q_wide.reshape(tok_count, wide_keyheads, -1, wide_width)
    k_wide = head_norm_rotate(
        keys_wide.reshape(tok_count, -1, wide_width), key_gain_wide, cos_wide, sin_wide
    )
    k_wide = k_wide.reshape(tok_count, -1)
    q_narrow = head_norm_rotate(
        queries_narrow.reshape(tok_count, -1, narrow_width),
        query_gain_narrow,
        cos_narrow,
        sin_narrow,
    )
    q_narrow = q_narrow.reshape(tok_count, narrow_keyheads, -1, narrow_width)
    k_narrow = head_norm_rotate(
        keys_narrow.reshape(tok_count, -1, narrow_width), key_gain_narrow, cos_narrow, sin_narrow
    )
    k_narrow = k_narrow.reshape(tok_count, -1)
    carried = (fresh_state(q_wide), fresh_state(q_narrow))
    carried = (
        key_sweep(
            carried[0],
            q_wide,
            lax.all_gather(k_wide, "sp", axis=0, tiled=True),
            lax.all_gather(values_wide, "sp", axis=0, tiled=True),
        ),
        key_sweep(
            carried[1],
            q_narrow,
            lax.all_gather(k_narrow, "sp", axis=0, tiled=True),
            lax.all_gather(values_narrow, "sp", axis=0, tiled=True),
        ),
    )
    heads_wide = finish_heads(carried[0])
    heads_narrow = finish_heads(carried[1])
    own_rows = residual.shape[0]
    mixed_heads = lax.psum_scatter(
        (
            jnp.dot(heads_wide, output_wide, preferred_element_type=jnp.float32)
            + jnp.dot(heads_narrow, output_narrow, preferred_element_type=jnp.float32)
        ).astype(jnp.bfloat16),
        "tp",
        scatter_dimension=0,
        tiled=True,
    ).astype(jnp.float32)
    attended = (residual.astype(jnp.float32) + mixed_heads).astype(jnp.bfloat16)
    state_float = attended.astype(jnp.float32)
    normed = (
        state_float
        * lax.rsqrt(jnp.mean(state_float * state_float, axis=-1, keepdims=True) + EPS)
        * norm_gain
    ).astype(jnp.bfloat16)
    pick_count = route_ids.shape[1]
    expert_count = lax.axis_size("sp")
    slot_count = 2 * pick_count * own_rows // expert_count
    model_width = residual.shape[1]
    own_tables = slot_tables(route_ids, slot_count, expert_count)
    send_rows = jnp.einsum(
        "rks,rd->sd", own_tables, normed, preferred_element_type=jnp.float32
    ).astype(jnp.bfloat16)
    send_rows = send_rows.reshape(expert_count, slot_count, model_width)
    arrived = lax.all_to_all(send_rows, "sp", split_axis=0, concat_axis=0, tiled=True)
    copies = lax.all_gather(arrived, "tp", axis=0, tiled=True)
    expert_arrived = copies.reshape((lax.axis_size("tp"),) + arrived.shape)
    full_shape = expert_arrived.shape
    flat_rows = expert_arrived.reshape(-1, model_width)
    gate_act = jnp.dot(flat_rows, gate_weight[0], preferred_element_type=jnp.float32)
    up_act = jnp.dot(flat_rows, up_weight[0], preferred_element_type=jnp.float32)
    hidden = (jax.nn.silu(gate_act) * up_act).astype(jnp.bfloat16)
    partial_value = jnp.dot(hidden, down_weight[0], preferred_element_type=jnp.float32).reshape(
        full_shape
    )
    summed = lax.psum_scatter(
        partial_value.astype(jnp.bfloat16), "tp", scatter_dimension=0, tiled=True
    ).astype(jnp.float32)
    results = summed.reshape(full_shape[1:]).astype(jnp.bfloat16)
    returned = lax.all_to_all(results, "sp", split_axis=0, concat_axis=0, tiled=True)
    returned_flat = returned.reshape(expert_count * slot_count, model_width)
    picked = jnp.einsum(
        "rks,sd->rkd", own_tables, returned_flat, preferred_element_type=jnp.float32
    )
    mixture = jnp.sum(route_weights[:, :, None] * picked, axis=1)
    return (state_float + mixture).astype(jnp.bfloat16)


LANES = 128
MESH_IDS = pl.DeviceIdType.MESH
PIECES = 2
ORDER = ((0, 1, 2, 3), (1, 0, 3, 2), (2, 3, 0, 1), (3, 2, 1, 0))


def pick(table, row, col):
    found = jnp.int32(0)
    for a in range(len(table)):
        for b in range(len(table[0])):
            found = jnp.where((row == a) & (col == b), jnp.int32(table[a][b]), found)
    return found


def remote(src, dst, send_sem, recv_sem, target):
    return pltpu.make_async_remote_copy(
        src_ref=src,
        dst_ref=dst,
        send_sem=send_sem,
        recv_sem=recv_sem,
        device_id=target,
        device_id_type=MESH_IDS,
    )


def lane_index(shape):
    return lax.broadcasted_iota(jnp.int32, shape, len(shape) - 1)


def turn_rotate(scaled, cos_table, sin_signed, quarter):
    lane = lane_index(scaled.shape)
    ahead = pltpu.roll(scaled, LANES - quarter, 1)
    behind = pltpu.roll(scaled, quarter, 1)
    return scaled * cos_table + jnp.where(lane % (2 * quarter) < quarter, ahead, behind) * sin_signed


def rotate_full(values, gain, cos_table, sin_signed):
    scaled = values * lax.rsqrt(jnp.mean(values * values, axis=-1, keepdims=True) + EPS) * gain
    return turn_rotate(scaled, cos_table, sin_signed, LANES // 4)


def rotate_half(values, gain, cos_table, sin_signed):
    half = LANES // 2
    low = lane_index(values.shape) < half
    square = values * values
    mean_low = jnp.sum(jnp.where(low, square, 0.0), axis=-1, keepdims=True) / half
    mean_high = jnp.sum(jnp.where(low, 0.0, square), axis=-1, keepdims=True) / half
    scaled = values * lax.rsqrt(jnp.where(low, mean_low, mean_high) + EPS) * gain
    return turn_rotate(scaled, cos_table, sin_signed, half // 4)


def fused_kernel(
    n_sp,
    n_tp,
    residual,
    queries_wide,
    keys_wide,
    values_wide,
    queries_narrow,
    keys_narrow,
    values_narrow,
    all_tables,
    query_gain_wide,
    key_gain_wide,
    query_gain_narrow,
    key_gain_narrow,
    norm_gain,
    routed,
    output_wide,
    output_narrow,
    gate_weight,
    up_weight,
    down_weight,
    result,
    kv,
    q_wide,
    q_narrow,
    top,
    total,
    mixed,
    heads,
    out_rows,
    term,
    term_in,
    term_sum,
    term_cross,
    attended,
    rows_all,
    gate_up,
    down,
    hidden,
    part,
    pair_in,
    cross_out,
    cross_in,
    single_out,
    single_in,
    double_out,
    double_in,
    last_out,
    last_in,
    tables,
    load_sem,
    kv_send,
    kv_recv,
    tp_send,
    tp_recv,
    ag_send,
    ag_recv,
    pair_send,
    pair_recv,
    cross_send,
    cross_recv,
    single_send,
    single_recv,
    double_send,
    double_recv,
    last_send,
    last_recv,
):
    me_s = lax.axis_index("sp")
    me_t = lax.axis_index("tp")
    core = me_t % 2
    column = me_t // 2
    partner = column * 2 + (1 - core)
    across = (1 - column) * 2 + core
    diagonal = (1 - column) * 2 + (1 - core)
    to_partner, to_across = {"tp": partner}, {"tp": across}
    has_left, has_right = me_s > 0, me_s < n_sp - 1
    to_left, to_right = {"sp": jnp.maximum(me_s - 1, 0)}, {"sp": jnp.minimum(me_s + 1, n_sp - 1)}
    near = [sorted(range(n_sp), key=lambda z: (abs(z - s), z)) for s in range(n_sp)]
    order = ORDER
    at_end = (me_s == 0) | (me_s == n_sp - 1)
    to_far = {"sp": jnp.where(me_s == 0, n_sp - 1, 0)}
    own = residual.shape[0]
    width = residual.shape[1]
    toks = queries_wide.shape[0]
    group = n_tp * own
    half = width // 2

    chunks = gate_weight.shape[2] // LANES
    table_load = pltpu.make_async_copy(
        all_tables.at[:, me_s], tables, load_sem.at[3 + 2 * chunks]
    )
    table_load.start()
    loads = [
        pltpu.make_async_copy(output_wide, out_rows.at[pl.ds(0, 2 * LANES)], load_sem.at[0]),
        pltpu.make_async_copy(output_narrow, out_rows.at[pl.ds(2 * LANES, LANES)], load_sem.at[1]),
        pltpu.make_async_copy(down_weight.at[0], down, load_sem.at[2]),
    ]
    for j in range(chunks):
        source = pl.ds(j * LANES, LANES)
        loads.append(
            pltpu.make_async_copy(
                gate_weight.at[0, :, source],
                gate_up.at[:, pl.ds(2 * j * LANES, LANES)],
                load_sem.at[3 + 2 * j],
            )
        )
        loads.append(
            pltpu.make_async_copy(
                up_weight.at[0, :, source],
                gate_up.at[:, pl.ds((2 * j + 1) * LANES, LANES)],
                load_sem.at[4 + 2 * j],
            )
        )
    barrier = pltpu.get_barrier_semaphore()
    pl.semaphore_signal(barrier, inc=1, device_id=to_partner, device_id_type=MESH_IDS)
    pl.semaphore_signal(barrier, inc=1, device_id=to_across, device_id_type=MESH_IDS)

    @pl.when(has_left)
    def _():
        pl.semaphore_signal(barrier, inc=1, device_id=to_left, device_id_type=MESH_IDS)

    @pl.when(has_right)
    def _():
        pl.semaphore_signal(barrier, inc=1, device_id=to_right, device_id_type=MESH_IDS)

    @pl.when(at_end)
    def _():
        pl.semaphore_signal(barrier, inc=1, device_id=to_far, device_id_type=MESH_IDS)

    table_load.wait()
    for load in loads:
        load.start()
    cos_wide, sin_wide = tables[0], tables[1]
    cos_narrow, sin_narrow = tables[2], tables[3]
    low = lane_index((toks, LANES)) < LANES // 2
    key_rot = rotate_full(keys_wide[...].astype(jnp.float32), key_gain_wide[...], cos_wide, sin_wide)
    kv[me_s, :, 0:LANES] = key_rot.astype(jnp.bfloat16)
    kv[me_s, :, LANES : 2 * LANES] = values_wide[...]
    packed = jnp.concatenate(
        [keys_narrow[...].astype(jnp.float32), values_narrow[...].astype(jnp.float32)], axis=0
    ).T
    packed_rot = rotate_half(packed, jnp.concatenate([key_gain_narrow[...]] * 2, axis=1), cos_narrow, sin_narrow)
    kv[me_s, :, 2 * LANES : 3 * LANES] = jnp.where(low, packed_rot, packed).astype(jnp.bfloat16)

    greeted = 4
    pl.semaphore_wait(barrier, greeted)

    def kv_copy(block, way, target):
        return remote(kv.at[block], kv.at[block], kv_send.at[way, block], kv_recv.at[block], target)

    @pl.when(has_right)
    def _():
        kv_copy(me_s, 0, to_right).start()

    @pl.when(has_left)
    def _():
        kv_copy(me_s, 1, to_left).start()

    for h in range(2):
        turned = rotate_full(
            queries_wide[:, h * LANES : (h + 1) * LANES].astype(jnp.float32),
            query_gain_wide[...],
            cos_wide,
            sin_wide,
        )
        q_wide[h * toks : (h + 1) * toks, :] = turned.astype(jnp.bfloat16)
    turned = rotate_half(
        queries_narrow[...].astype(jnp.float32), jnp.concatenate([query_gain_narrow[...]] * 2, axis=1), cos_narrow, sin_narrow
    )
    q_narrow[0:toks, :] = jnp.where(low, turned, 0.0).astype(jnp.bfloat16)
    q_narrow[toks : 2 * toks, :] = jnp.where(
        low, pltpu.roll(turned, LANES // 2, 1), 0.0
    ).astype(jnp.bfloat16)
    top[...] = jnp.full(top.shape, NEG_BIG, jnp.float32)
    total[...] = jnp.zeros(total.shape, jnp.float32)
    mixed[...] = jnp.zeros(mixed.shape, jnp.float32)

    def sweep(kind, queries, keys, values, scale):
        scores = lax.dot_general(
            queries, keys, (((1,), (1,)), ((), ())), preferred_element_type=jnp.float32
        )
        old_top = top[kind]
        new_top = jnp.maximum(old_top, jnp.max(scores, axis=-1, keepdims=True))
        weights = jnp.exp((scores - new_top) * scale)
        rescale = jnp.exp((old_top - new_top) * scale)
        total[kind] = total[kind] * rescale + jnp.sum(weights, axis=-1, keepdims=True)
        mixed[kind] = mixed[kind] * rescale + jnp.dot(
            weights.astype(jnp.bfloat16), values, preferred_element_type=jnp.float32
        )
        top[kind] = new_top

    def attend_step(i, carry):
        block = pick(near, me_s, i)
        sweep(
            0,
            q_wide[...],
            kv[block, :, 0:LANES],
            kv[block, :, LANES : 2 * LANES],
            LANES**-0.5,
        )
        both = kv[block, :, 2 * LANES : 3 * LANES]
        sweep(1, q_narrow[...], both, both, (LANES // 2) ** -0.5)
        lower, upper = me_s - (i + 1), me_s + (i + 1)

        @pl.when(lower >= 0)
        def _():
            kv_copy(lower, 0, to_right).wait_recv()

            @pl.when(has_right)
            def _():
                kv_copy(lower, 0, to_right).start()

        @pl.when(upper < n_sp)
        def _():
            kv_copy(upper, 1, to_left).wait_recv()

            @pl.when(has_left)
            def _():
                kv_copy(upper, 1, to_left).start()

        return carry

    lax.fori_loop(0, n_sp, attend_step, 0)

    head_wide = mixed[0] / total[0]
    head_narrow = mixed[1] / total[1]
    heads[:, 0:LANES] = head_wide[0:toks].astype(jnp.bfloat16)
    heads[:, LANES : 2 * LANES] = head_wide[toks : 2 * toks].astype(jnp.bfloat16)
    heads[:, 2 * LANES : 3 * LANES] = jnp.where(
        low, pltpu.roll(head_narrow[0:toks], LANES // 2, 1), head_narrow[toks : 2 * toks]
    ).astype(jnp.bfloat16)
    loads[0].wait()
    loads[1].wait()

    def project(dest):
        term[dest] = jnp.dot(
            heads[pl.ds(pl.multiple_of(dest * own, own), own), :],
            out_rows[...],
            preferred_element_type=jnp.float32,
        ).astype(jnp.bfloat16)

    def pair_term(place, dest):
        return remote(
            term.at[dest], term_in.at[place], tp_send.at[place], tp_recv.at[place], to_partner
        )

    cross_term = remote(term_sum, term_cross, tp_send.at[2], tp_recv.at[2], to_across)
    project(diagonal)
    pair_term(0, diagonal).start()
    project(across)
    project(partner)
    pair_term(1, partner).start()
    project(me_t)
    pair_term(0, diagonal).wait_recv()
    term_sum[...] = (
        term[across].astype(jnp.float32) + term_in[0].astype(jnp.float32)
    ).astype(jnp.bfloat16)
    cross_term.start()
    pair_term(1, partner).wait_recv()
    state = (
        residual[...].astype(jnp.float32)
        + term[me_t].astype(jnp.float32)
        + term_in[1].astype(jnp.float32)
    )
    cross_term.wait_recv()
    state = (state + term_cross[...].astype(jnp.float32)).astype(jnp.bfloat16)
    attended[...] = state
    state = state.astype(jnp.float32)
    normed = (
        state
        * lax.rsqrt(jnp.mean(state * state, axis=-1, keepdims=True) + EPS)
        * norm_gain[...]
    ).astype(jnp.bfloat16)
    rows_all[me_s, me_t, :, 0:width] = normed
    rows_all[me_s, me_t, :, width : width + LANES] = routed[...]
    piece_rows = own // PIECES

    def spread(z, t, way, k, target):
        rows = rows_all.at[z, t, pl.ds(k * piece_rows, piece_rows)]
        return remote(rows, rows, ag_send.at[z, way, k], ag_recv.at[z, t, k], target)

    for k in range(PIECES):
        spread(me_s, me_t, 2, k, to_across).start()

        @pl.when(has_right)
        def _():
            spread(me_s, me_t, 0, k, to_right).start()

        @pl.when(has_left)
        def _():
            spread(me_s, me_t, 1, k, to_left).start()

        spread(me_s, me_t, 3, k, to_partner).start()
    for load in loads[2:]:
        load.wait()

    def pair_part(z, side, dest):
        return remote(
            part.at[z, dest],
            pair_in.at[z, side],
            pair_send.at[z, side],
            pair_recv.at[z, side],
            to_partner,
        )

    def own_sum(z, h):
        return part[z, me_t, h].astype(jnp.float32) + pair_in[z, 1, h].astype(jnp.float32)

    def across_sum(z, h):
        return part[z, across, h].astype(jnp.float32) + pair_in[z, 0, h].astype(jnp.float32)

    def cross_part(z):
        return remote(cross_out.at[z], cross_in.at[z], cross_send.at[z], cross_recv.at[z], to_across)

    def reach(z):
        gap = jnp.abs(z - me_s)
        ahead = z > me_s
        slot = jnp.where(
            gap == 2, jnp.where(ahead, 2, 3), jnp.where(ahead == (gap == 1), 0, 1)
        )
        return slot, {"sp": jnp.where(gap == 2, (z + me_s) // 2, z)}

    def single(z):
        slot, target = reach(z)
        return remote(
            single_out.at[z], single_in.at[slot], single_send.at[z], single_recv.at[slot], target
        )

    def double(z, side):
        slot, target = reach(z)
        return remote(
            double_out.at[z, side],
            double_in.at[slot, side],
            double_send.at[z, side],
            double_recv.at[slot, side],
            target,
        )

    def single_arrived(slot):
        remote(
            single_out.at[0], single_in.at[slot], single_send.at[0], single_recv.at[slot], to_left
        ).wait_recv()

    def double_arrived(slot, side):
        remote(
            double_out.at[0, side],
            double_in.at[slot, side],
            double_send.at[0, side],
            double_recv.at[slot, side],
            to_left,
        ).wait_recv()

    has_mid = has_left & has_right

    def relayed(z):
        return has_mid & (jnp.abs(z - me_s) == 1)

    def combine_own(z):
        pair_part(z, 1, partner).wait_recv()

        @pl.when((z != me_s) & jnp.logical_not(relayed(z)))
        def _():
            double_out[z, 0] = own_sum(z, 1).astype(jnp.bfloat16)
            double(z, 0).start()

    def combine_across(z):
        pair_part(z, 0, diagonal).wait_recv()
        cross_out[z] = across_sum(z, 0).astype(jnp.bfloat16)
        cross_part(z).start()

        @pl.when((z != me_s) & jnp.logical_not(relayed(z)))
        def _():
            double_out[z, 1] = across_sum(z, 1).astype(jnp.bfloat16)
            double(z, 1).start()

    def launch(z):
        @pl.when((z != me_s) & jnp.logical_not(relayed(z)))
        def _():
            cross_part(z).wait_recv()
            single_out[z] = (own_sum(z, 0) + cross_in[z].astype(jnp.float32)).astype(jnp.bfloat16)
            single(z).start()

    lane = lane_index((2 * own, LANES))
    mine = (lane < 3 * n_sp) & (lane % n_sp == me_s)

    def expert_half(z, col):
        rows = rows_all.at[z, pl.ds(2 * col, 2)]
        weight = jnp.sum(
            jnp.where(
                mine,
                rows[:, :, width : width + LANES].astype(jnp.float32).reshape(2 * own, LANES),
                0.0,
            ),
            axis=-1,
            keepdims=True,
        )
        inputs = rows[:, :, 0:width].reshape(2 * own, width)
        for j in range(chunks):
            act = jnp.dot(
                inputs,
                gate_up[:, 2 * j * LANES : 2 * (j + 1) * LANES],
                preferred_element_type=jnp.float32,
            )
            gate_act, up_act = act[:, 0:LANES], act[:, LANES : 2 * LANES]
            hidden[:, j * LANES : (j + 1) * LANES] = (
                gate_act / (1.0 + jnp.exp(-gate_act)) * up_act
            ).astype(jnp.bfloat16)
        for j in range(width // (2 * LANES)):
            piece = jnp.dot(
                hidden[...],
                down[:, 2 * j * LANES : 2 * (j + 1) * LANES],
                preferred_element_type=jnp.float32,
            )
            side = j // (half // (2 * LANES))
            start = 2 * j * LANES - side * half
            part[z, pl.ds(2 * col, 2), side, :, start : start + 2 * LANES] = (
                (piece * weight).astype(jnp.bfloat16).reshape(2, own, 2 * LANES)
            )

    def expert_step(step, carry):
        i, k = step // 2, step % 2
        z = pick(order, me_s, i)
        lower, upper = me_s - (i + 1), me_s + (i + 1)

        @pl.when(lower >= 0)
        def _():
            spread(lower, me_t, 0, k, to_right).wait_recv()

            @pl.when(has_right)
            def _():
                spread(lower, me_t, 0, k, to_right).start()

            spread(lower, me_t, 3, k, to_partner).start()

        @pl.when(upper < n_sp)
        def _():
            spread(upper, me_t, 1, k, to_left).wait_recv()

            @pl.when(has_left)
            def _():
                spread(upper, me_t, 1, k, to_left).start()

            spread(upper, me_t, 3, k, to_partner).start()

        @pl.when(i < n_sp - 1)
        def _():
            spread(pick(order, me_s, jnp.minimum(i + 1, n_sp - 1)), me_t, 2, k, to_across).start()

        spread(z, across, 4, k, to_partner).wait_recv()
        spread(z, across, 4, k, to_partner).start()

        @pl.when(k == 0)
        def _():
            for p in range(PIECES):
                spread(z, partner, 3, p, to_partner).wait_recv()

        @pl.when(k == 1)
        def _():
            combine_own(z)

            @pl.when(i >= 2)
            def _():
                combine_across(pick(order, me_s, i - 1))

        @pl.when(k == 1)
        def _():
            for p in range(PIECES):
                spread(z, diagonal, 3, p, to_partner).wait_recv()

        expert_half(z, jnp.where(k == 0, column, 1 - column))
        pair_part(z, 1 - k, jnp.where(k == 0, partner, diagonal)).start()
        return carry

    lax.fori_loop(0, 2 * n_sp, expert_step, 0)
    launch(pick(order, me_s, 1))
    combine_across(pick(order, me_s, n_sp - 1))
    combine_across(me_s)
    launch(pick(order, me_s, n_sp - 2))
    def pass_double(z, slot):
        double_arrived(slot, 0)
        double_out[z, 0] = (own_sum(z, 1) + double_in[slot, 0].astype(jnp.float32)).astype(
            jnp.bfloat16
        )
        double(z, 0).start()
        double_arrived(slot, 1)
        double_out[z, 1] = (across_sum(z, 1) + double_in[slot, 1].astype(jnp.float32)).astype(
            jnp.bfloat16
        )
        double(z, 1).start()

    def pass_single(z, slot):
        cross_part(z).wait_recv()
        single_arrived(slot)
        single_out[z] = (
            own_sum(z, 0)
            + cross_in[z].astype(jnp.float32)
            + single_in[slot].astype(jnp.float32)
        ).astype(jnp.bfloat16)
        single(z).start()

    @pl.when(has_mid)
    def _():
        for z, slot in ((me_s + 1, 2), (me_s - 1, 3)):
            pass_double(z, slot)
        for z, slot in ((me_s + 1, 2), (me_s - 1, 3)):
            pass_single(z, slot)

    launch(pick(order, me_s, n_sp - 1))

    last_cross = remote(last_out, last_in, last_send.at[0], last_recv.at[0], to_across)
    for slot in range(2):
        for side in range(2):
            double_arrived(slot, side)
    last_out[...] = (
        across_sum(me_s, 1)
        + double_in[0, 1].astype(jnp.float32)
        + double_in[1, 1].astype(jnp.float32)
    ).astype(jnp.bfloat16)
    last_cross.start()
    cross_part(me_s).wait_recv()
    single_arrived(0)
    single_arrived(1)
    result[:, 0:half] = (
        attended[:, 0:half].astype(jnp.float32)
        + own_sum(me_s, 0)
        + cross_in[me_s].astype(jnp.float32)
        + single_in[0].astype(jnp.float32)
        + single_in[1].astype(jnp.float32)
    ).astype(jnp.bfloat16)
    partial = (
        attended[:, half:width].astype(jnp.float32)
        + own_sum(me_s, 1)
        + double_in[0, 0].astype(jnp.float32)
        + double_in[1, 0].astype(jnp.float32)
    )
    last_cross.wait_recv()
    result[:, half:width] = (partial + last_in[...].astype(jnp.float32)).astype(jnp.bfloat16)

    pair_term(0, diagonal).wait_send()
    pair_term(1, partner).wait_send()
    cross_term.wait_send()
    last_cross.wait_send()

    def drain(z, carry):
        cross_part(z).wait_send()
        pair_part(z, 0, diagonal).wait_send()
        pair_part(z, 1, partner).wait_send()
        for k in range(PIECES):
            spread(z, me_t, 2, k, to_across).wait_send()
            spread(z, me_t, 3, k, to_partner).wait_send()
            spread(z, across, 4, k, to_partner).wait_send()

        @pl.when((z <= me_s) & has_right)
        def _():
            kv_copy(z, 0, to_right).wait_send()
            for k in range(PIECES):
                spread(z, me_t, 0, k, to_right).wait_send()

        @pl.when((z >= me_s) & has_left)
        def _():
            kv_copy(z, 1, to_left).wait_send()
            for k in range(PIECES):
                spread(z, me_t, 1, k, to_left).wait_send()

        @pl.when(z != me_s)
        def _():
            single(z).wait_send()
            double(z, 0).wait_send()
            double(z, 1).wait_send()

        return carry

    lax.fori_loop(0, n_sp, drain, 0)


def signed_tables(tok_count, head_width):
    places = np.arange(tok_count, dtype=np.int32)
    quarter = head_width // 4
    inv_freq = np.float32(THETA) ** (-np.arange(quarter, dtype=np.float32) / np.float32(quarter))
    row_angle = (places // GRID).astype(np.float32)[:, None] * inv_freq[None, :]
    col_angle = (places % GRID).astype(np.float32)[:, None] * inv_freq[None, :]
    angles = np.concatenate([row_angle, row_angle, col_angle, col_angle], axis=-1)
    sign = np.where(np.arange(head_width) % (2 * quarter) < quarter, -1.0, 1.0)
    cos_table, sin_table = np.cos(angles), np.sin(angles) * sign.astype(np.float32)
    copies = LANES // head_width
    return [np.tile(table, (1, copies)).astype(np.float32) for table in (cos_table, sin_table)]


def fused_body(
    residual,
    queries_wide,
    keys_wide,
    values_wide,
    queries_narrow,
    keys_narrow,
    values_narrow,
    query_gain_wide,
    key_gain_wide,
    query_gain_narrow,
    key_gain_narrow,
    output_wide,
    output_narrow,
    norm_gain,
    gate_weight,
    up_weight,
    down_weight,
    route_ids,
    route_weights,
):
    n_sp, n_tp = lax.axis_size("sp"), lax.axis_size("tp")
    own, width = residual.shape
    toks = queries_wide.shape[0]
    half = width // 2
    units = gate_weight.shape[2]
    whole = n_sp * toks
    tables = np.stack(
        signed_tables(whole, query_gain_wide.shape[0])
        + signed_tables(whole, query_gain_narrow.shape[0])
    )
    tables = jnp.asarray(tables.reshape(4, n_sp, toks, LANES))
    lane = jnp.arange(LANES, dtype=jnp.int32)[None, :]
    dense = jnp.zeros((own, LANES), jnp.float32)
    for k in range(route_ids.shape[1]):
        dense += jnp.where(route_ids[:, k : k + 1] == lane % n_sp, route_weights[:, k : k + 1], 0.0)
    first = lax.reduce_precision(dense, 8, 7)
    second = lax.reduce_precision(dense - first, 8, 7)
    third = dense - first - second
    routed = jnp.where(lane < n_sp, first, jnp.where(lane < 2 * n_sp, second, third))
    routed = jnp.where(lane < 3 * n_sp, routed, 0.0).astype(jnp.bfloat16)
    vmem = pl.BlockSpec(memory_space=pltpu.VMEM)
    anywhere = pl.BlockSpec(memory_space=pl.ANY)
    low_type, full_type = jnp.bfloat16, jnp.float32
    dma = pltpu.SemaphoreType.DMA
    scratch = [
        pltpu.VMEM((n_sp, toks, 3 * LANES), low_type),
        pltpu.VMEM((2 * toks, LANES), low_type),
        pltpu.VMEM((2 * toks, LANES), low_type),
        pltpu.VMEM((2, 2 * toks, 1), full_type),
        pltpu.VMEM((2, 2 * toks, 1), full_type),
        pltpu.VMEM((2, 2 * toks, LANES), full_type),
        pltpu.VMEM((toks, 3 * LANES), low_type),
        pltpu.VMEM((3 * LANES, width), low_type),
        pltpu.VMEM((n_tp, own, width), low_type),
        pltpu.VMEM((2, own, width), low_type),
        pltpu.VMEM((own, width), low_type),
        pltpu.VMEM((own, width), low_type),
        pltpu.VMEM((own, width), low_type),
        pltpu.VMEM((n_sp, n_tp, own, width + LANES), low_type),
        pltpu.VMEM((width, 2 * units), low_type),
        pltpu.VMEM((units, width), low_type),
        pltpu.VMEM((2 * own, units), low_type),
        pltpu.VMEM((n_sp, n_tp, 2, own, half), low_type),
        pltpu.VMEM((n_sp, 2, 2, own, half), low_type),
        pltpu.VMEM((n_sp, own, half), low_type),
        pltpu.VMEM((n_sp, own, half), low_type),
        pltpu.VMEM((n_sp, own, half), low_type),
        pltpu.VMEM((4, own, half), low_type),
        pltpu.VMEM((n_sp, 2, own, half), low_type),
        pltpu.VMEM((4, 2, own, half), low_type),
        pltpu.VMEM((own, half), low_type),
        pltpu.VMEM((own, half), low_type),
        pltpu.VMEM((4, toks, LANES), full_type),
        dma((4 + 2 * (units // LANES),)),
        dma((2, n_sp)),
        dma((n_sp,)),
        dma((3,)),
        dma((3,)),
        dma((n_sp, 5, PIECES)),
        dma((n_sp, n_tp, PIECES)),
        dma((n_sp, 2)),
        dma((n_sp, 2)),
        dma((n_sp,)),
        dma((n_sp,)),
        dma((n_sp,)),
        dma((4,)),
        dma((n_sp, 2)),
        dma((4, 2)),
        dma((1,)),
        dma((1,)),
    ]
    return pl.pallas_call(
        functools.partial(fused_kernel, n_sp, n_tp),
        out_shape=jax.ShapeDtypeStruct(residual.shape, residual.dtype),
        in_specs=[vmem] * 7 + [anywhere] + [vmem] * 6 + [anywhere] * 5,
        out_specs=vmem,
        scratch_shapes=scratch,
        compiler_params=pltpu.CompilerParams(
            collective_id=0, has_side_effects=True, vmem_limit_bytes=60 * 1024 * 1024
        ),
        name="fused_layer",
    )(
        residual,
        queries_wide,
        keys_wide,
        values_wide,
        queries_narrow,
        keys_narrow.T,
        values_narrow.T,
        tables,
        query_gain_wide.reshape(1, LANES),
        key_gain_wide.reshape(1, LANES),
        query_gain_narrow.reshape(1, LANES // 2),
        key_gain_narrow.reshape(1, LANES // 2),
        norm_gain.reshape(1, width),
        routed,
        output_wide,
        output_narrow,
        gate_weight,
        up_weight,
        down_weight,
    )


def body(*operands):
    residual, queries_wide, keys_wide = operands[0], operands[1], operands[2]
    queries_narrow, keys_narrow = operands[4], operands[5]
    wide_width, narrow_width = operands[7].shape[0], operands[9].shape[0]
    n_sp, n_tp = lax.axis_size("sp"), lax.axis_size("tp")
    own = residual.shape[0]
    fits = (
        n_tp == 4
        and n_sp == len(ORDER)
        and 2 * operands[17].shape[1] * own // n_sp >= own
        and wide_width == LANES
        and narrow_width == LANES // 2
        and queries_wide.shape[1] == 2 * LANES
        and keys_wide.shape[1] == LANES
        and queries_narrow.shape[1] == LANES
        and keys_narrow.shape[1] == LANES // 2
        and queries_wide.shape[0] == n_tp * own
        and own % (16 * PIECES) == 0
    )
    return fused_body(*operands) if fits else plain_body(*operands)


def solution(mesh):
    return jax.shard_map(
        body,
        mesh=mesh,
        in_specs=(
            P(("grp", "sp", "tp"), None),
            P(("grp", "sp"), "tp"),
            P(("grp", "sp"), "tp"),
            P(("grp", "sp"), "tp"),
            P(("grp", "sp"), "tp"),
            P(("grp", "sp"), "tp"),
            P(("grp", "sp"), "tp"),
            P(),
            P(),
            P(),
            P(),
            P("tp", None),
            P("tp", None),
            P(),
            P("sp", None, "tp"),
            P("sp", None, "tp"),
            P("sp", "tp", None),
            P(("grp", "sp", "tp"), None),
            P(("grp", "sp", "tp"), None),
        ),
        out_specs=P(("grp", "sp", "tp"), None),
        check_vma=False,
    )
```

```python
import functools

import jax
import jax.numpy as jnp
import numpy as np
from jax import lax
from jax.experimental import pallas as pl
from jax.experimental.pallas import tpu as pltpu
from jax.sharding import PartitionSpec as P

GRID = 64


THETA = 10000.0
EPS = 1e-06
NEG_BIG = -1e30


def rotary_tables(places, head_width):
    quarter = head_width // 4
    inv_freq = THETA ** (-jnp.arange(quarter, dtype=jnp.float32) / quarter)
    grid_rows = (places // GRID).astype(jnp.float32)
    grid_cols = (places % GRID).astype(jnp.float32)
    row_angle = grid_rows[:, None] * inv_freq[None, :]
    col_angle = grid_cols[:, None] * inv_freq[None, :]
    angles = jnp.concatenate([row_angle, row_angle, col_angle, col_angle], axis=-1)
    return (jnp.cos(angles), jnp.sin(angles))


def head_norm_rotate(values, gain_vec, cos_table, sin_table):
    as_float = values.astype(jnp.float32)
    scaled = as_float * lax.rsqrt(jnp.mean(as_float * as_float, axis=-1, keepdims=True) + EPS)
    scaled = scaled * gain_vec
    full_shape = scaled.shape
    quarter = full_shape[-1] // 4
    halves = scaled.reshape(full_shape[:-1] + (2, 2, quarter))
    turned = jnp.stack([-halves[..., 1, :], halves[..., 0, :]], axis=-2).reshape(full_shape)
    return (scaled * cos_table[:, None, :] + turned * sin_table[:, None, :]).astype(jnp.bfloat16)


def fresh_state(queries):
    key_heads, group_size, tok_count = (queries.shape[1], queries.shape[2], queries.shape[0])
    return (
        jnp.full((key_heads, group_size, tok_count), NEG_BIG, jnp.float32),
        jnp.zeros((key_heads, group_size, tok_count), jnp.float32),
        jnp.zeros(queries.shape, jnp.float32),
    )


def key_sweep(carried, queries, keys, values):
    key_count = keys.shape[0]
    key_heads = queries.shape[1]
    head_width = queries.shape[3]
    block_len = 2048 if key_count % 2048 == 0 else key_count
    key_blocks = keys.reshape(key_count // block_len, block_len, key_heads, head_width)
    value_blocks = values.reshape(key_count // block_len, block_len, key_heads, head_width)
    score_scale = head_width ** (-0.5)

    def step(carried_state, blocks_in):
        key_block, value_block = blocks_in
        running_max, weight_sum, weighted = carried_state
        scores = (
            jnp.einsum("qhgd,khd->hgqk", queries, key_block, preferred_element_type=jnp.float32)
            * score_scale
        )
        new_max = jnp.maximum(running_max, jnp.max(scores, axis=-1))
        weights = jnp.exp(scores - new_max[..., None])
        rescale = jnp.exp(running_max - new_max)
        weight_sum = weight_sum * rescale + jnp.sum(weights, axis=-1)
        mixed_values = jnp.einsum(
            "hgqk,khd->qhgd",
            weights.astype(jnp.bfloat16),
            value_block,
            preferred_element_type=jnp.float32,
        )
        weighted = weighted * jnp.transpose(rescale, (2, 0, 1))[..., None] + mixed_values
        return ((new_max, weight_sum, weighted), None)

    carried, _ = lax.scan(step, carried, (key_blocks, value_blocks))
    return carried


def finish_heads(carried):
    weighted = carried[2]
    outcome = weighted / jnp.transpose(carried[1], (2, 0, 1))[..., None]
    return outcome.astype(jnp.bfloat16).reshape(weighted.shape[0], -1)


def slot_tables(chosen, slot_count, expert_count):
    row_count = chosen.shape[0]
    pick_count = chosen.shape[1]
    flat_pick = chosen.reshape(row_count * pick_count)
    hit_marks = (flat_pick[:, None] == jnp.arange(expert_count, dtype=jnp.int32)[None, :]).astype(
        jnp.int32
    )
    before = jnp.cumsum(hit_marks, axis=0) - hit_marks
    slot_place = jnp.sum(before * hit_marks, axis=1)
    target = flat_pick * slot_count + slot_place
    slot_table = target[:, None] == jnp.arange(expert_count * slot_count, dtype=jnp.int32)[None, :]
    return slot_table.astype(jnp.bfloat16).reshape(row_count, pick_count, expert_count * slot_count)


def plain_body(
    residual,
    queries_wide,
    keys_wide,
    values_wide,
    queries_narrow,
    keys_narrow,
    values_narrow,
    query_gain_wide,
    key_gain_wide,
    query_gain_narrow,
    key_gain_narrow,
    output_wide,
    output_narrow,
    norm_gain,
    gate_weight,
    up_weight,
    down_weight,
    route_ids,
    route_weights,
):
    tok_count = queries_wide.shape[0]
    places = lax.axis_index("sp") * tok_count + jnp.arange(tok_count, dtype=jnp.int32)
    wide_width = query_gain_wide.shape[0]
    narrow_width = query_gain_narrow.shape[0]
    cos_wide, sin_wide = rotary_tables(places, wide_width)
    cos_narrow, sin_narrow = rotary_tables(places, narrow_width)
    wide_keyheads = keys_wide.shape[1] // wide_width
    narrow_keyheads = keys_narrow.shape[1] // narrow_width
    q_wide = head_norm_rotate(
        queries_wide.reshape(tok_count, -1, wide_width), query_gain_wide, cos_wide, sin_wide
    )
    q_wide = q_wide.reshape(tok_count, wide_keyheads, -1, wide_width)
    k_wide = head_norm_rotate(
        keys_wide.reshape(tok_count, -1, wide_width), key_gain_wide, cos_wide, sin_wide
    )
    k_wide = k_wide.reshape(tok_count, -1)
    q_narrow = head_norm_rotate(
        queries_narrow.reshape(tok_count, -1, narrow_width),
        query_gain_narrow,
        cos_narrow,
        sin_narrow,
    )
    q_narrow = q_narrow.reshape(tok_count, narrow_keyheads, -1, narrow_width)
    k_narrow = head_norm_rotate(
        keys_narrow.reshape(tok_count, -1, narrow_width), key_gain_narrow, cos_narrow, sin_narrow
    )
    k_narrow = k_narrow.reshape(tok_count, -1)
    carried = (fresh_state(q_wide), fresh_state(q_narrow))
    carried = (
        key_sweep(
            carried[0],
            q_wide,
            lax.all_gather(k_wide, "sp", axis=0, tiled=True),
            lax.all_gather(values_wide, "sp", axis=0, tiled=True),
        ),
        key_sweep(
            carried[1],
            q_narrow,
            lax.all_gather(k_narrow, "sp", axis=0, tiled=True),
            lax.all_gather(values_narrow, "sp", axis=0, tiled=True),
        ),
    )
    heads_wide = finish_heads(carried[0])
    heads_narrow = finish_heads(carried[1])
    own_rows = residual.shape[0]
    mixed_heads = lax.psum_scatter(
        (
            jnp.dot(heads_wide, output_wide, preferred_element_type=jnp.float32)
            + jnp.dot(heads_narrow, output_narrow, preferred_element_type=jnp.float32)
        ).astype(jnp.bfloat16),
        "tp",
        scatter_dimension=0,
        tiled=True,
    ).astype(jnp.float32)
    attended = (residual.astype(jnp.float32) + mixed_heads).astype(jnp.bfloat16)
    state_float = attended.astype(jnp.float32)
    normed = (
        state_float
        * lax.rsqrt(jnp.mean(state_float * state_float, axis=-1, keepdims=True) + EPS)
        * norm_gain
    ).astype(jnp.bfloat16)
    pick_count = route_ids.shape[1]
    expert_count = lax.axis_size("sp")
    slot_count = 2 * pick_count * own_rows // expert_count
    model_width = residual.shape[1]
    own_tables = slot_tables(route_ids, slot_count, expert_count)
    send_rows = jnp.einsum(
        "rks,rd->sd", own_tables, normed, preferred_element_type=jnp.float32
    ).astype(jnp.bfloat16)
    send_rows = send_rows.reshape(expert_count, slot_count, model_width)
    arrived = lax.all_to_all(send_rows, "sp", split_axis=0, concat_axis=0, tiled=True)
    copies = lax.all_gather(arrived, "tp", axis=0, tiled=True)
    expert_arrived = copies.reshape((lax.axis_size("tp"),) + arrived.shape)
    full_shape = expert_arrived.shape
    flat_rows = expert_arrived.reshape(-1, model_width)
    gate_act = jnp.dot(flat_rows, gate_weight[0], preferred_element_type=jnp.float32)
    up_act = jnp.dot(flat_rows, up_weight[0], preferred_element_type=jnp.float32)
    hidden = (jax.nn.silu(gate_act) * up_act).astype(jnp.bfloat16)
    partial_value = jnp.dot(hidden, down_weight[0], preferred_element_type=jnp.float32).reshape(
        full_shape
    )
    summed = lax.psum_scatter(
        partial_value.astype(jnp.bfloat16), "tp", scatter_dimension=0, tiled=True
    ).astype(jnp.float32)
    results = summed.reshape(full_shape[1:]).astype(jnp.bfloat16)
    returned = lax.all_to_all(results, "sp", split_axis=0, concat_axis=0, tiled=True)
    returned_flat = returned.reshape(expert_count * slot_count, model_width)
    picked = jnp.einsum(
        "rks,sd->rkd", own_tables, returned_flat, preferred_element_type=jnp.float32
    )
    mixture = jnp.sum(route_weights[:, :, None] * picked, axis=1)
    return (state_float + mixture).astype(jnp.bfloat16)


LANES = 128
MESH_IDS = pl.DeviceIdType.MESH
PIECES = 2
LEAD_PARTS = 4
ORDER = ((0, 1, 2, 3), (1, 0, 3, 2), (2, 3, 0, 1), (3, 2, 1, 0))


def pick(table, row, col):
    found = jnp.int32(0)
    for a in range(len(table)):
        for b in range(len(table[0])):
            found = jnp.where((row == a) & (col == b), jnp.int32(table[a][b]), found)
    return found


def remote(src, dst, send_sem, recv_sem, target):
    return pltpu.make_async_remote_copy(
        src_ref=src,
        dst_ref=dst,
        send_sem=send_sem,
        recv_sem=recv_sem,
        device_id=target,
        device_id_type=MESH_IDS,
    )


def lane_index(shape):
    return lax.broadcasted_iota(jnp.int32, shape, len(shape) - 1)


def turn_rotate(scaled, cos_table, sin_signed, quarter):
    lane = lane_index(scaled.shape)
    ahead = pltpu.roll(scaled, LANES - quarter, 1)
    behind = pltpu.roll(scaled, quarter, 1)
    return scaled * cos_table + jnp.where(lane % (2 * quarter) < quarter, ahead, behind) * sin_signed


def rotate_full(values, gain, cos_table, sin_signed):
    scaled = values * lax.rsqrt(jnp.mean(values * values, axis=-1, keepdims=True) + EPS) * gain
    return turn_rotate(scaled, cos_table, sin_signed, LANES // 4)


def rotate_half(values, gain, cos_table, sin_signed):
    half = LANES // 2
    low = lane_index(values.shape) < half
    square = values * values
    mean_low = jnp.sum(jnp.where(low, square, 0.0), axis=-1, keepdims=True) / half
    mean_high = jnp.sum(jnp.where(low, 0.0, square), axis=-1, keepdims=True) / half
    scaled = values * lax.rsqrt(jnp.where(low, mean_low, mean_high) + EPS) * gain
    return turn_rotate(scaled, cos_table, sin_signed, half // 4)


def fused_kernel(
    n_sp,
    n_tp,
    residual,
    queries_wide,
    keys_wide,
    values_wide,
    queries_narrow,
    keys_narrow,
    values_narrow,
    all_tables,
    query_gain_wide,
    key_gain_wide,
    query_gain_narrow,
    key_gain_narrow,
    norm_gain,
    route_ids,
    route_weights,
    output_wide,
    output_narrow,
    gate_weight,
    up_weight,
    down_weight,
    result,
    kv,
    q_wide,
    q_narrow,
    top,
    total,
    mixed,
    heads,
    out_rows,
    term,
    term_in,
    term_sum,
    term_cross,
    attended,
    rows_all,
    gate_up,
    down,
    hidden,
    part,
    pair_in,
    cross_out,
    cross_in,
    single_out,
    single_in,
    double_out,
    double_in,
    last_out,
    last_in,
    tables,
    weights,
    load_sem,
    kv_send,
    kv_recv,
    share_send,
    share_recv,
    spread_send,
    spread_recv,
    tp_send,
    tp_recv,
    ag_send,
    ag_recv,
    pair_send,
    pair_recv,
    cross_send,
    cross_recv,
    single_send,
    single_recv,
    double_send,
    double_recv,
    last_send,
    last_recv,
):
    me_s = lax.axis_index("sp")
    me_t = lax.axis_index("tp")
    core = me_t % 2
    column = me_t // 2
    partner = column * 2 + (1 - core)
    across = (1 - column) * 2 + core
    diagonal = (1 - column) * 2 + (1 - core)
    to_partner, to_across = {"tp": partner}, {"tp": across}
    has_left, has_right = me_s > 0, me_s < n_sp - 1
    to_left, to_right = {"sp": jnp.maximum(me_s - 1, 0)}, {"sp": jnp.minimum(me_s + 1, n_sp - 1)}
    near = [sorted(range(n_sp), key=lambda z: (abs(z - s), z)) for s in range(n_sp)]
    order = ORDER
    at_end = (me_s == 0) | (me_s == n_sp - 1)
    to_far = {"sp": jnp.where(me_s == 0, n_sp - 1, 0)}
    own = residual.shape[0]
    width = residual.shape[1]
    toks = queries_wide.shape[0]
    group = n_tp * own
    split = width * LEAD_PARTS // 8
    n_experts = weights.shape[2]

    chunks = gate_weight.shape[2] // LANES
    table_load = pltpu.make_async_copy(
        all_tables.at[:, me_s], tables, load_sem.at[3 + 2 * chunks]
    )
    table_load.start()
    loads = [
        pltpu.make_async_copy(output_wide, out_rows.at[pl.ds(0, 2 * LANES)], load_sem.at[0]),
        pltpu.make_async_copy(output_narrow, out_rows.at[pl.ds(2 * LANES, LANES)], load_sem.at[1]),
        pltpu.make_async_copy(down_weight.at[0], down, load_sem.at[2]),
    ]
    for j in range(chunks):
        source = pl.ds(j * LANES, LANES)
        loads.append(
            pltpu.make_async_copy(
                gate_weight.at[0, :, source],
                gate_up.at[:, pl.ds(2 * j * LANES, LANES)],
                load_sem.at[3 + 2 * j],
            )
        )
        loads.append(
            pltpu.make_async_copy(
                up_weight.at[0, :, source],
                gate_up.at[:, pl.ds((2 * j + 1) * LANES, LANES)],
                load_sem.at[4 + 2 * j],
            )
        )
    barrier = pltpu.get_barrier_semaphore()
    pl.semaphore_signal(barrier, inc=1, device_id=to_partner, device_id_type=MESH_IDS)
    pl.semaphore_signal(barrier, inc=1, device_id=to_across, device_id_type=MESH_IDS)

    @pl.when(has_left)
    def _():
        pl.semaphore_signal(barrier, inc=1, device_id=to_left, device_id_type=MESH_IDS)

    @pl.when(has_right)
    def _():
        pl.semaphore_signal(barrier, inc=1, device_id=to_right, device_id_type=MESH_IDS)

    @pl.when(at_end)
    def _():
        pl.semaphore_signal(barrier, inc=1, device_id=to_far, device_id_type=MESH_IDS)

    kv[me_s, 0] = values_wide[...]
    expert = lax.broadcasted_iota(jnp.int32, (n_experts, own), 0)
    shares = jnp.zeros((n_experts, own), jnp.float32)
    for k in range(route_ids.shape[0]):
        shares += jnp.where(route_ids[k : k + 1, :] == expert, route_weights[k : k + 1, :], 0.0)
    weights[me_s, me_t] = jnp.concatenate([shares, jnp.zeros_like(shares)], axis=1)
    pl.semaphore_wait(barrier, 4)

    def kv_copy(block, p, way, target):
        return remote(
            kv.at[block, p],
            kv.at[block, p],
            kv_send.at[way, block, p],
            kv_recv.at[block, p],
            target,
        )

    def share_copy(block, way, target):
        return remote(
            weights.at[block, me_t],
            weights.at[block, me_t],
            share_send.at[way, block],
            share_recv.at[block],
            target,
        )

    def send_kv(p):
        @pl.when(has_right)
        def _():
            kv_copy(me_s, p, 0, to_right).start()

        @pl.when(has_left)
        def _():
            kv_copy(me_s, p, 1, to_left).start()

    send_kv(0)
    table_load.wait()
    for load in loads:
        load.start()
    cos_wide, sin_wide = tables[0], tables[1]
    cos_narrow, sin_narrow = tables[2], tables[3]
    low = lane_index((toks, LANES)) < LANES // 2
    key_rot = rotate_full(keys_wide[...].astype(jnp.float32), key_gain_wide[...], cos_wide, sin_wide)
    kv[me_s, 1] = key_rot.astype(jnp.bfloat16)
    send_kv(1)
    packed = jnp.concatenate(
        [keys_narrow[...].astype(jnp.float32), values_narrow[...].astype(jnp.float32)], axis=0
    ).T
    packed_rot = rotate_half(packed, jnp.concatenate([key_gain_narrow[...]] * 2, axis=1), cos_narrow, sin_narrow)
    kv[me_s, 2] = jnp.where(low, packed_rot, packed).astype(jnp.bfloat16)
    send_kv(2)

    @pl.when(has_right)
    def _():
        share_copy(me_s, 0, to_right).start()

    @pl.when(has_left)
    def _():
        share_copy(me_s, 1, to_left).start()

    for h in range(2):
        turned = rotate_full(
            queries_wide[:, h * LANES : (h + 1) * LANES].astype(jnp.float32),
            query_gain_wide[...],
            cos_wide,
            sin_wide,
        )
        q_wide[h * toks : (h + 1) * toks, :] = turned.astype(jnp.bfloat16)
    turned = rotate_half(
        queries_narrow[...].astype(jnp.float32), jnp.concatenate([query_gain_narrow[...]] * 2, axis=1), cos_narrow, sin_narrow
    )
    q_narrow[0:toks, :] = jnp.where(low, turned, 0.0).astype(jnp.bfloat16)
    q_narrow[toks : 2 * toks, :] = jnp.where(
        low, pltpu.roll(turned, LANES // 2, 1), 0.0
    ).astype(jnp.bfloat16)
    top[...] = jnp.full(top.shape, NEG_BIG, jnp.float32)
    total[...] = jnp.zeros(total.shape, jnp.float32)
    mixed[...] = jnp.zeros(mixed.shape, jnp.float32)

    def sweep(kind, queries, keys, values, scale):
        scores = lax.dot_general(
            queries, keys, (((1,), (1,)), ((), ())), preferred_element_type=jnp.float32
        )
        old_top = top[kind]
        new_top = jnp.maximum(old_top, jnp.max(scores, axis=-1, keepdims=True))
        weights = jnp.exp((scores - new_top) * scale)
        rescale = jnp.exp((old_top - new_top) * scale)
        total[kind] = total[kind] * rescale + jnp.sum(weights, axis=-1, keepdims=True)
        mixed[kind] = mixed[kind] * rescale + jnp.dot(
            weights.astype(jnp.bfloat16), values, preferred_element_type=jnp.float32
        )
        top[kind] = new_top

    def attend_wide(block):
        sweep(0, q_wide[...], kv[block, 1], kv[block, 0], LANES**-0.5)

    def attend_narrow(block):
        both = kv[block, 2]
        sweep(1, q_narrow[...], both, both, (LANES // 2) ** -0.5)

    attend_wide(me_s)
    attend_narrow(me_s)

    def attend_step(i, carry):
        block = pick(near, me_s, i)
        lower, upper = me_s - i, me_s + i

        def kv_pass(p):
            @pl.when(lower >= 0)
            def _():
                kv_copy(lower, p, 0, to_right).wait_recv()

                @pl.when(has_right)
                def _():
                    kv_copy(lower, p, 0, to_right).start()

            @pl.when(upper < n_sp)
            def _():
                kv_copy(upper, p, 1, to_left).wait_recv()

                @pl.when(has_left)
                def _():
                    kv_copy(upper, p, 1, to_left).start()

        kv_pass(0)
        kv_pass(1)
        attend_wide(block)
        kv_pass(2)
        attend_narrow(block)

        @pl.when(lower >= 0)
        def _():
            share_copy(lower, 0, to_right).wait_recv()

            @pl.when(has_right)
            def _():
                share_copy(lower, 0, to_right).start()

        @pl.when(upper < n_sp)
        def _():
            share_copy(upper, 1, to_left).wait_recv()

            @pl.when(has_left)
            def _():
                share_copy(upper, 1, to_left).start()

        return carry

    lax.fori_loop(1, n_sp, attend_step, 0)

    def share_spread(t, way, target):
        return remote(
            weights.at[:, t], weights.at[:, t], spread_send.at[way], spread_recv.at[t], target
        )

    head_wide = mixed[0] / total[0]
    head_narrow = mixed[1] / total[1]
    heads[:, 0:LANES] = head_wide[0:toks].astype(jnp.bfloat16)
    heads[:, LANES : 2 * LANES] = head_wide[toks : 2 * toks].astype(jnp.bfloat16)
    heads[:, 2 * LANES : 3 * LANES] = jnp.where(
        low, pltpu.roll(head_narrow[0:toks], LANES // 2, 1), head_narrow[toks : 2 * toks]
    ).astype(jnp.bfloat16)
    loads[0].wait()
    loads[1].wait()

    piece_rows = own // PIECES

    def project(col):
        place = pl.ds(pl.multiple_of(2 * col * own, 2 * own), 2 * own)
        term[pl.ds(2 * col, 2)] = (
            jnp.dot(heads[place, :], out_rows[...], preferred_element_type=jnp.float32)
            .astype(jnp.bfloat16)
            .reshape(2, own, width)
        )

    def rows_of(k):
        return pl.ds(k * piece_rows, piece_rows)

    def pair_term(place, dest, k):
        return remote(
            term.at[dest, rows_of(k)],
            term_in.at[place, rows_of(k)],
            tp_send.at[place, k],
            tp_recv.at[place, k],
            to_partner,
        )

    def cross_term(k):
        return remote(
            term_sum.at[rows_of(k)],
            term_cross.at[rows_of(k)],
            tp_send.at[2, k],
            tp_recv.at[2, k],
            to_across,
        )

    project(1 - column)
    for k in range(PIECES):
        pair_term(0, diagonal, k).start()
    project(column)
    for k in range(PIECES):
        pair_term(1, partner, k).start()
    for k in range(PIECES):
        pair_term(0, diagonal, k).wait_recv()
        term_sum[rows_of(k)] = (
            term[across, rows_of(k)].astype(jnp.float32)
            + term_in[0, rows_of(k)].astype(jnp.float32)
        ).astype(jnp.bfloat16)
        cross_term(k).start()
    share_spread(me_t, 0, to_across).start()
    share_spread(me_t, 1, to_partner).start()
    def spread(z, t, way, k, target):
        rows = rows_all.at[z, t, rows_of(k)]
        return remote(rows, rows, ag_send.at[z, way, k], ag_recv.at[z, t, k], target)

    for k in range(PIECES):
        pair_term(1, partner, k).wait_recv()
        cross_term(k).wait_recv()
        state = (
            residual[rows_of(k), :].astype(jnp.float32)
            + term[me_t, rows_of(k)].astype(jnp.float32)
            + term_in[1, rows_of(k)].astype(jnp.float32)
            + term_cross[rows_of(k)].astype(jnp.float32)
        ).astype(jnp.bfloat16)
        attended[rows_of(k), :] = state
        state = state.astype(jnp.float32)
        rows_all[me_s, me_t, rows_of(k)] = (
            state
            * lax.rsqrt(jnp.mean(state * state, axis=-1, keepdims=True) + EPS)
            * norm_gain[...]
        ).astype(jnp.bfloat16)
        spread(me_s, me_t, 2, k, to_across).start()

        @pl.when(has_right)
        def _():
            spread(me_s, me_t, 0, k, to_right).start()

        @pl.when(has_left)
        def _():
            spread(me_s, me_t, 1, k, to_left).start()

        spread(me_s, me_t, 3, k, to_partner).start()
    share_spread(across, 2, to_partner).wait_recv()
    share_spread(across, 2, to_partner).start()
    share_spread(partner, 1, to_partner).wait_recv()
    share_spread(diagonal, 1, to_partner).wait_recv()
    for load in loads[2:]:
        load.wait()

    def pair_part(z, side, dest):
        return remote(
            part.at[z, dest],
            pair_in.at[z, side],
            pair_send.at[z, side],
            pair_recv.at[z, side],
            to_partner,
        )

    lead = pl.ds(0, split)
    rest = pl.ds(split, width - split)

    def own_sum(z, columns):
        return part[z, me_t, :, columns].astype(jnp.float32) + pair_in[z, 1, :, columns].astype(
            jnp.float32
        )

    def across_sum(z, columns):
        return part[z, across, :, columns].astype(jnp.float32) + pair_in[
            z, 0, :, columns
        ].astype(jnp.float32)

    def cross_part(z):
        return remote(cross_out.at[z], cross_in.at[z], cross_send.at[z], cross_recv.at[z], to_across)

    def reach(z):
        gap = jnp.abs(z - me_s)
        ahead = z > me_s
        slot = jnp.where(
            gap == 2, jnp.where(ahead, 2, 3), jnp.where(ahead == (gap == 1), 0, 1)
        )
        return slot, {"sp": jnp.where(gap == 2, (z + me_s) // 2, z)}

    def single(z):
        slot, target = reach(z)
        return remote(
            single_out.at[z], single_in.at[slot], single_send.at[z], single_recv.at[slot], target
        )

    def double(z, side):
        slot, target = reach(z)
        return remote(
            double_out.at[z, side],
            double_in.at[slot, side],
            double_send.at[z, side],
            double_recv.at[slot, side],
            target,
        )

    def single_arrived(slot):
        remote(
            single_out.at[0], single_in.at[slot], single_send.at[0], single_recv.at[slot], to_left
        ).wait_recv()

    def double_arrived(slot, side):
        remote(
            double_out.at[0, side],
            double_in.at[slot, side],
            double_send.at[0, side],
            double_recv.at[slot, side],
            to_left,
        ).wait_recv()

    has_mid = has_left & has_right

    def relayed(z):
        return has_mid & (jnp.abs(z - me_s) == 1)

    def double_start(z, side):
        pair_sum = across_sum(z, rest) if side else own_sum(z, rest)
        double_out[z, side] = pair_sum.astype(jnp.bfloat16)
        double(z, side).start()

    def double_pass(z, side):
        slot = jnp.where(z > me_s, 2, 3)
        double_arrived(slot, side)
        pair_sum = across_sum(z, rest) if side else own_sum(z, rest)
        double_out[z, side] = (pair_sum + double_in[slot, side].astype(jnp.float32)).astype(
            jnp.bfloat16
        )
        double(z, side).start()

    def cross_start(z):
        cross_out[z] = across_sum(z, lead).astype(jnp.bfloat16)
        cross_part(z).start()

    def single_start(z):
        cross_part(z).wait_recv()
        single_out[z] = (own_sum(z, lead) + cross_in[z].astype(jnp.float32)).astype(jnp.bfloat16)
        single(z).start()

    def single_pass(z):
        slot = jnp.where(z > me_s, 2, 3)
        cross_part(z).wait_recv()
        single_arrived(slot)
        single_out[z] = (
            own_sum(z, lead)
            + cross_in[z].astype(jnp.float32)
            + single_in[slot].astype(jnp.float32)
        ).astype(jnp.bfloat16)
        single(z).start()

    def expert_half(z, col):
        pair = weights.at[z, pl.ds(2 * col, 2)]
        low_lane = lane_index((n_experts, LANES)) < own
        by_token = jnp.where(low_lane, pair[0], pltpu.roll(pair[1], LANES - own, 1)).T
        weight = jnp.sum(
            jnp.where(lane_index(by_token.shape) == me_s, by_token, 0.0), axis=-1, keepdims=True
        )
        inputs = rows_all[z, pl.ds(2 * col, 2)].reshape(2 * own, width)
        for j in range(chunks):
            act = jnp.dot(
                inputs,
                gate_up[:, 2 * j * LANES : 2 * (j + 1) * LANES],
                preferred_element_type=jnp.float32,
            )
            gate_act, up_act = act[:, 0:LANES], act[:, LANES : 2 * LANES]
            hidden[:, j * LANES : (j + 1) * LANES] = (
                gate_act / (1.0 + jnp.exp(-gate_act)) * up_act
            ).astype(jnp.bfloat16)
        for j in range(width // (2 * LANES)):
            columns = slice(2 * j * LANES, 2 * (j + 1) * LANES)
            piece = jnp.dot(hidden[...], down[:, columns], preferred_element_type=jnp.float32)
            part[z, pl.ds(2 * col, 2), :, columns] = (
                (piece * weight).astype(jnp.bfloat16).reshape(2, own, 2 * LANES)
            )

    def expert_step(step, carry):
        i, k = step // 2, step % 2
        z = pick(order, me_s, i)
        lower, upper = me_s - (i + 1), me_s + (i + 1)

        @pl.when(lower >= 0)
        def _():
            spread(lower, me_t, 0, k, to_right).wait_recv()

            @pl.when(has_right)
            def _():
                spread(lower, me_t, 0, k, to_right).start()

            spread(lower, me_t, 3, k, to_partner).start()

        @pl.when(upper < n_sp)
        def _():
            spread(upper, me_t, 1, k, to_left).wait_recv()

            @pl.when(has_left)
            def _():
                spread(upper, me_t, 1, k, to_left).start()

            spread(upper, me_t, 3, k, to_partner).start()

        @pl.when(i < n_sp - 1)
        def _():
            spread(pick(order, me_s, jnp.minimum(i + 1, n_sp - 1)), me_t, 2, k, to_across).start()

        spread(z, across, 4, k, to_partner).wait_recv()
        spread(z, across, 4, k, to_partner).start()

        @pl.when(k == 0)
        def _():
            for p in range(PIECES):
                spread(z, partner, 3, p, to_partner).wait_recv()

        before = pick(order, me_s, jnp.maximum(i - 1, 0))

        @pl.when((k == 0) & (i >= 2))
        def _():
            pair_part(before, 0, diagonal).wait_recv()

            @pl.when(jnp.logical_not(relayed(before)))
            def _():
                double_start(before, 1)

        @pl.when(k == 1)
        def _():
            pair_part(z, 1, partner).wait_recv()

            @pl.when((i >= 1) & jnp.logical_not(relayed(z)))
            def _():
                double_start(z, 0)

            @pl.when(i >= 2)
            def _():
                cross_start(before)

            @pl.when((i == n_sp - 1) & has_mid)
            def _():
                double_pass(pick(order, me_s, 1), 0)
                double_pass(z, 0)

        @pl.when(k == 1)
        def _():
            for p in range(PIECES):
                spread(z, diagonal, 3, p, to_partner).wait_recv()

        expert_half(z, jnp.where(k == 0, column, 1 - column))
        pair_part(z, 1 - k, jnp.where(k == 0, partner, diagonal)).start()
        return carry

    lax.fori_loop(0, 2 * n_sp, expert_step, 0)
    first, second, third = (pick(order, me_s, jnp.int32(i)) for i in range(1, n_sp))

    @pl.when(jnp.logical_not(has_mid))
    def _():
        single_start(first)

    pair_part(third, 0, diagonal).wait_recv()
    cross_start(third)

    @pl.when(jnp.logical_not(has_mid))
    def _():
        double_start(third, 1)

    @pl.when(has_mid)
    def _():
        double_pass(first, 1)

    single_start(second)

    @pl.when(has_mid)
    def _():
        double_pass(third, 1)

    pair_part(me_s, 0, diagonal).wait_recv()
    cross_start(me_s)

    @pl.when(has_mid)
    def _():
        single_pass(first)
        single_pass(third)

    @pl.when(jnp.logical_not(has_mid))
    def _():
        single_start(third)

    last_cross = remote(last_out, last_in, last_send.at[0], last_recv.at[0], to_across)
    for slot in range(2):
        for side in range(2):
            double_arrived(slot, side)
    last_out[...] = (
        across_sum(me_s, rest)
        + double_in[0, 1].astype(jnp.float32)
        + double_in[1, 1].astype(jnp.float32)
    ).astype(jnp.bfloat16)
    last_cross.start()
    cross_part(me_s).wait_recv()
    single_arrived(0)
    single_arrived(1)
    result[:, lead] = (
        attended[:, lead].astype(jnp.float32)
        + own_sum(me_s, lead)
        + cross_in[me_s].astype(jnp.float32)
        + single_in[0].astype(jnp.float32)
        + single_in[1].astype(jnp.float32)
    ).astype(jnp.bfloat16)
    partial = (
        attended[:, rest].astype(jnp.float32)
        + own_sum(me_s, rest)
        + double_in[0, 0].astype(jnp.float32)
        + double_in[1, 0].astype(jnp.float32)
    )
    last_cross.wait_recv()
    result[:, rest] = (partial + last_in[...].astype(jnp.float32)).astype(jnp.bfloat16)

    for k in range(PIECES):
        pair_term(0, diagonal, k).wait_send()
        pair_term(1, partner, k).wait_send()
        cross_term(k).wait_send()
    share_spread(me_t, 0, to_across).wait_send()
    share_spread(me_t, 1, to_partner).wait_send()
    share_spread(across, 2, to_partner).wait_send()
    last_cross.wait_send()

    def drain(z, carry):
        cross_part(z).wait_send()
        pair_part(z, 0, diagonal).wait_send()
        pair_part(z, 1, partner).wait_send()
        for k in range(PIECES):
            spread(z, me_t, 2, k, to_across).wait_send()
            spread(z, me_t, 3, k, to_partner).wait_send()
            spread(z, across, 4, k, to_partner).wait_send()

        @pl.when((z <= me_s) & has_right)
        def _():
            for p in range(3):
                kv_copy(z, p, 0, to_right).wait_send()
            share_copy(z, 0, to_right).wait_send()
            for k in range(PIECES):
                spread(z, me_t, 0, k, to_right).wait_send()

        @pl.when((z >= me_s) & has_left)
        def _():
            for p in range(3):
                kv_copy(z, p, 1, to_left).wait_send()
            share_copy(z, 1, to_left).wait_send()
            for k in range(PIECES):
                spread(z, me_t, 1, k, to_left).wait_send()

        @pl.when(z != me_s)
        def _():
            single(z).wait_send()
            double(z, 0).wait_send()
            double(z, 1).wait_send()

        return carry

    lax.fori_loop(0, n_sp, drain, 0)


def signed_tables(tok_count, head_width):
    places = np.arange(tok_count, dtype=np.int32)
    quarter = head_width // 4
    inv_freq = np.float32(THETA) ** (-np.arange(quarter, dtype=np.float32) / np.float32(quarter))
    row_angle = (places // GRID).astype(np.float32)[:, None] * inv_freq[None, :]
    col_angle = (places % GRID).astype(np.float32)[:, None] * inv_freq[None, :]
    angles = np.concatenate([row_angle, row_angle, col_angle, col_angle], axis=-1)
    sign = np.where(np.arange(head_width) % (2 * quarter) < quarter, -1.0, 1.0)
    cos_table, sin_table = np.cos(angles), np.sin(angles) * sign.astype(np.float32)
    copies = LANES // head_width
    return [np.tile(table, (1, copies)).astype(np.float32) for table in (cos_table, sin_table)]


def fused_body(
    residual,
    queries_wide,
    keys_wide,
    values_wide,
    queries_narrow,
    keys_narrow,
    values_narrow,
    query_gain_wide,
    key_gain_wide,
    query_gain_narrow,
    key_gain_narrow,
    output_wide,
    output_narrow,
    norm_gain,
    gate_weight,
    up_weight,
    down_weight,
    route_ids,
    route_weights,
):
    n_sp, n_tp = lax.axis_size("sp"), lax.axis_size("tp")
    own, width = residual.shape
    toks = queries_wide.shape[0]
    split = width * LEAD_PARTS // 8
    units = gate_weight.shape[2]
    whole = n_sp * toks
    tables = np.stack(
        signed_tables(whole, query_gain_wide.shape[0])
        + signed_tables(whole, query_gain_narrow.shape[0])
    )
    tables = jnp.asarray(tables.reshape(4, n_sp, toks, LANES))
    vmem = pl.BlockSpec(memory_space=pltpu.VMEM)
    anywhere = pl.BlockSpec(memory_space=pl.ANY)
    low_type, full_type = jnp.bfloat16, jnp.float32
    dma = pltpu.SemaphoreType.DMA
    scratch = [
        pltpu.VMEM((n_sp, 3, toks, LANES), low_type),
        pltpu.VMEM((2 * toks, LANES), low_type),
        pltpu.VMEM((2 * toks, LANES), low_type),
        pltpu.VMEM((2, 2 * toks, 1), full_type),
        pltpu.VMEM((2, 2 * toks, 1), full_type),
        pltpu.VMEM((2, 2 * toks, LANES), full_type),
        pltpu.VMEM((toks, 3 * LANES), low_type),
        pltpu.VMEM((3 * LANES, width), low_type),
        pltpu.VMEM((n_tp, own, width), low_type),
        pltpu.VMEM((2, own, width), low_type),
        pltpu.VMEM((own, width), low_type),
        pltpu.VMEM((own, width), low_type),
        pltpu.VMEM((own, width), low_type),
        pltpu.VMEM((n_sp, n_tp, own, width), low_type),
        pltpu.VMEM((width, 2 * units), low_type),
        pltpu.VMEM((units, width), low_type),
        pltpu.VMEM((2 * own, units), low_type),
        pltpu.VMEM((n_sp, n_tp, own, width), low_type),
        pltpu.VMEM((n_sp, 2, own, width), low_type),
        pltpu.VMEM((n_sp, own, split), low_type),
        pltpu.VMEM((n_sp, own, split), low_type),
        pltpu.VMEM((n_sp, own, split), low_type),
        pltpu.VMEM((4, own, split), low_type),
        pltpu.VMEM((n_sp, 2, own, width - split), low_type),
        pltpu.VMEM((4, 2, own, width - split), low_type),
        pltpu.VMEM((own, width - split), low_type),
        pltpu.VMEM((own, width - split), low_type),
        pltpu.VMEM((4, toks, LANES), full_type),
        pltpu.VMEM((n_sp, n_tp, 8, LANES), full_type),
        dma((4 + 2 * (units // LANES),)),
        dma((2, n_sp, 3)),
        dma((n_sp, 3)),
        dma((2, n_sp)),
        dma((n_sp,)),
        dma((3,)),
        dma((n_tp,)),
        dma((3, PIECES)),
        dma((3, PIECES)),
        dma((n_sp, 5, PIECES)),
        dma((n_sp, n_tp, PIECES)),
        dma((n_sp, 2)),
        dma((n_sp, 2)),
        dma((n_sp,)),
        dma((n_sp,)),
        dma((n_sp,)),
        dma((4,)),
        dma((n_sp, 2)),
        dma((4, 2)),
        dma((1,)),
        dma((1,)),
    ]
    return pl.pallas_call(
        functools.partial(fused_kernel, n_sp, n_tp),
        out_shape=jax.ShapeDtypeStruct(residual.shape, residual.dtype),
        in_specs=[vmem] * 7 + [anywhere] + [vmem] * 7 + [anywhere] * 5,
        out_specs=vmem,
        scratch_shapes=scratch,
        compiler_params=pltpu.CompilerParams(
            collective_id=0, has_side_effects=True, vmem_limit_bytes=60 * 1024 * 1024
        ),
        name="fused_layer",
    )(
        residual,
        queries_wide,
        keys_wide,
        values_wide,
        queries_narrow,
        keys_narrow.T,
        values_narrow.T,
        tables,
        query_gain_wide.reshape(1, LANES),
        key_gain_wide.reshape(1, LANES),
        query_gain_narrow.reshape(1, LANES // 2),
        key_gain_narrow.reshape(1, LANES // 2),
        norm_gain.reshape(1, width),
        route_ids.T,
        route_weights.T,
        output_wide,
        output_narrow,
        gate_weight,
        up_weight,
        down_weight,
    )


def body(*operands):
    residual, queries_wide, keys_wide = operands[0], operands[1], operands[2]
    queries_narrow, keys_narrow = operands[4], operands[5]
    wide_width, narrow_width = operands[7].shape[0], operands[9].shape[0]
    n_sp, n_tp = lax.axis_size("sp"), lax.axis_size("tp")
    own = residual.shape[0]
    fits = (
        n_tp == 4
        and n_sp == len(ORDER)
        and 2 * own == LANES
        and 2 * operands[17].shape[1] * own // n_sp >= own
        and wide_width == LANES
        and narrow_width == LANES // 2
        and queries_wide.shape[1] == 2 * LANES
        and keys_wide.shape[1] == LANES
        and queries_narrow.shape[1] == LANES
        and keys_narrow.shape[1] == LANES // 2
        and queries_wide.shape[0] == n_tp * own
        and own % (16 * PIECES) == 0
    )
    return fused_body(*operands) if fits else plain_body(*operands)


def solution(mesh):
    return jax.shard_map(
        body,
        mesh=mesh,
        in_specs=(
            P(("grp", "sp", "tp"), None),
            P(("grp", "sp"), "tp"),
            P(("grp", "sp"), "tp"),
            P(("grp", "sp"), "tp"),
            P(("grp", "sp"), "tp"),
            P(("grp", "sp"), "tp"),
            P(("grp", "sp"), "tp"),
            P(),
            P(),
            P(),
            P(),
            P("tp", None),
            P("tp", None),
            P(),
            P("sp", None, "tp"),
            P("sp", None, "tp"),
            P("sp", "tp", None),
            P(("grp", "sp", "tp"), None),
            P(("grp", "sp", "tp"), None),
        ),
        out_specs=P(("grp", "sp", "tp"), None),
        check_vma=False,
    )
```
